32 devices in a mesh: sp: 8 (over z, y), tp: 4 (over x, core).
Axes of the slice: x: 2, y: 2, z: 4, core: 2. Of those that a mesh axis runs over, the one named last changes fastest.
Arguments:
- frames: bfloat16 [4, 1024, 1024], P('tp', 'sp'), may hold values from -22 to 22
- norm_gain: float32 [1024], replicated, may hold values from 0.5 to 1.5
- conv_value_w: bfloat16 [1024, 512], P(None, 'tp'), may hold values from -0.1875 to 0.1875
- conv_gate_w: bfloat16 [1024, 512], P(None, 'tp'), may hold values from -0.1875 to 0.1875
- conv_taps: bfloat16 [31, 512], P(None, 'tp'), may hold values from -1 to 1
- conv_bias: float32 [512], P('tp'), may hold values from -1.2 to 1.2
- channel_gain: float32 [512], P('tp'), may hold values from 0.5 to 1.5
- channel_shift: float32 [512], P('tp'), may hold values from -1.2 to 1.2
- query_w: bfloat16 [1024, 1024], P(None, 'tp'), may hold values from -0.1875 to 0.1875
- forget_w: bfloat16 [1024, 1024], P(None, 'tp'), may hold values from -0.1875 to 0.1875
- input_w: bfloat16 [1024, 1024], P(None, 'tp'), may hold values from -0.1875 to 0.1875
- gate_w: bfloat16 [1024, 1024], P(None, 'tp'), may hold values from -0.1875 to 0.1875
- memory_rate: float32 [1024], P('tp'), may hold values from 0.5 to 32
- head_gain: float32 [1024], P('tp'), may hold values from 0.5 to 1.5
- conv_out_w: bfloat16 [512, 1024], P('tp'), may hold values from -0.1875 to 0.1875
- rec_out_w: bfloat16 [1024, 1024], P('tp'), may hold values from -0.125 to 0.125
Outputs:
- mixed: bfloat16 [4, 1024, 1024], P('tp', 'sp')
The draws below stay inside these ranges and needn't reach their ends.
All inputs are finite; a program needn't handle non-finite values.
Results may differ from the reference program's by a relative error of at most 0.015.
The reference program's roundings to bfloat16 on the way (of `normed`, `gated_conv`, `conv_out`, `scores`, `carried_low` and `rec_out`) count: a program that leaves them out, or rounds other values in their place, can miss the bound.
Values may be sent and summed in bfloat16 or wider, within the bound.
A program may use at most 64 MiB of HBM per device.

```python
import math
import jax
import jax.numpy as jnp
from jax import lax

D = 1024
D_CONV = 512
CONV_WIDTH = 31
HEADS = 8
HEAD = 128
D_HG = 1024
POS_DEV = 128
SEQS = 4
SEQ_LEN = 1024
N_SP = 8


def draw_frames(key, part):
    noise_key = jax.random.fold_in(key, 11)
    direction_key = jax.random.fold_in(key, 12)
    level_key = jax.random.fold_in(key, 13)
    block_count = SEQ_LEN // POS_DEV
    noise = jnp.clip(jax.random.normal(noise_key, (SEQS, SEQ_LEN, D), jnp.float32), -6.0, 6.0)
    direction = jnp.clip(jax.random.normal(direction_key, (D,), jnp.float32), -4.0, 4.0)
    levels = jax.random.uniform(level_key, (SEQS, block_count, 1, 1), jnp.float32, -4.0, 4.0)
    spread_levels = jnp.broadcast_to(levels, (SEQS, block_count, POS_DEV, 1)).reshape(SEQS, SEQ_LEN, 1)
    return (noise + spread_levels * direction).astype(jnp.bfloat16)


def shard_levels(stream_key, extent, pieces, low, largest):
    def one(dim, blocks):
        draws = jax.random.uniform(jax.random.fold_in(jax.random.fold_in(stream_key, 6), dim), (blocks,), jnp.float32, low / len(pieces), largest / len(pieces))
        return jnp.repeat(jnp.exp(draws), extent[dim] // blocks).reshape((-1,) + (1,) * (len(extent) - dim - 1))

    gain = one(*pieces[0])
    for cut in pieces[1:]:
        gain = gain * one(*cut)
    return gain


def bell_draw(key, dims, deviation, most, shards=(), held_as=jnp.bfloat16):
    values = deviation * jax.random.normal(key, dims, jnp.float32)
    if shards:
        values = values * shard_levels(key, dims, shards, -0.22, 0.18)
    return jnp.clip(values, -most, most).astype(held_as)


def setup_inputs(seed: int = 0) -> dict:
    arg_keys = jax.random.split(jax.random.key(seed), 17)
    return {
        "frames": draw_frames(jax.random.fold_in(arg_keys[16], 71), 0),
        "norm_gain": jnp.clip(1.0 + 0.1 * jax.random.normal(arg_keys[1], (D,), jnp.float32), 0.5, 1.5),
        "conv_value_w": bell_draw(arg_keys[2], (D, D_CONV), D ** -0.5, 0.1875, ((1, 4),)),
        "conv_gate_w": bell_draw(arg_keys[3], (D, D_CONV), D ** -0.5, 0.1875, ((1, 4),)),
        "conv_taps": bell_draw(arg_keys[4], (CONV_WIDTH, D_CONV), CONV_WIDTH ** -0.5, 1.0, ((1, 4),)),
        "conv_bias": bell_draw(arg_keys[5], (D_CONV,), 0.2, 1.2, ((0, 4),), jnp.float32),
        "channel_gain": jnp.clip(1.0 + 0.1 * jax.random.normal(arg_keys[6], (D_CONV,), jnp.float32), 0.5, 1.5),
        "channel_shift": bell_draw(arg_keys[7], (D_CONV,), 0.2, 1.2, ((0, 4),), jnp.float32),
        "query_w": bell_draw(arg_keys[8], (D, D_HG), D ** -0.5, 0.1875, ((1, 4),)),
        "forget_w": bell_draw(arg_keys[9], (D, D_HG), D ** -0.5, 0.1875, ((1, 4),)),
        "input_w": bell_draw(arg_keys[10], (D, D_HG), D ** -0.5, 0.1875, ((1, 4),)),
        "gate_w": bell_draw(arg_keys[11], (D, D_HG), D ** -0.5, 0.1875, ((1, 4),)),
        "memory_rate": jnp.clip(jnp.exp(math.log(32.0) - 4.158883 * jax.random.uniform(arg_keys[12], (D_HG,), jnp.float32) ** shard_levels(arg_keys[12], (D_HG,), ((0, 4),), -0.2, 0.2)), 0.5, 32.0),
        "head_gain": jnp.clip(1.0 + 0.1 * jax.random.normal(arg_keys[13], (D_HG,), jnp.float32), 0.5, 1.5),
        "conv_out_w": bell_draw(arg_keys[14], (D_CONV, D), (2 * D_CONV) ** -0.5, 0.1875, ((0, 4),)),
        "rec_out_w": bell_draw(arg_keys[15], (D_HG, D), (2 * D_HG) ** -0.5, 0.125, ((0, 4),)),
    }


EPS = 1e-06

def reference(frames, norm_gain, conv_value_w, conv_gate_w, conv_taps, conv_bias, channel_gain, channel_shift, query_w, forget_w, input_w, gate_w, memory_rate, head_gain, conv_out_w, rec_out_w):
    values = frames.astype(jnp.float32)
    normed = (values * lax.rsqrt(lax.optimization_barrier(jnp.mean(values * values, axis=-1, keepdims=True)) + EPS) * norm_gain).astype(jnp.bfloat16)
    flat_rows = normed.reshape(SEQS * SEQ_LEN, D)

    def project(weight):
        product = jnp.dot(flat_rows, weight, preferred_element_type=jnp.float32)
        return product.astype(jnp.bfloat16).reshape(SEQS, SEQ_LEN, weight.shape[1])
    conv_value = project(conv_value_w)
    conv_gate = project(conv_gate_w)
    queries = project(query_w)
    forget_raw = project(forget_w)
    inputs = project(input_w)
    out_gate = project(gate_w)
    gated_conv = (conv_value.astype(jnp.float32) * jax.nn.sigmoid(conv_gate.astype(jnp.float32))).astype(jnp.bfloat16)
    filtered = lax.conv_general_dilated(gated_conv, conv_taps[:, None, :], window_strides=(1,), padding=[(CONV_WIDTH - 1, 0)], dimension_numbers=('NWC', 'WIO', 'NWC'), feature_group_count=D_CONV, preferred_element_type=jnp.float32) + conv_bias
    row_mean = lax.optimization_barrier(jnp.mean(filtered, axis=-1, keepdims=True))
    row_var = lax.optimization_barrier(jnp.mean(filtered * filtered, axis=-1, keepdims=True)) - row_mean * row_mean
    scaled = (filtered - row_mean) * lax.rsqrt(row_var + EPS) * channel_gain + channel_shift
    conv_out = jax.nn.silu(scaled).astype(jnp.bfloat16)
    head_shape = (SEQS, SEQ_LEN, HEADS, HEAD)
    rate_rows = (memory_rate / SEQ_LEN).reshape(HEADS, HEAD)
    in_gate = rate_rows * jax.nn.sigmoid(-forget_raw.astype(jnp.float32)).reshape(head_shape)
    log_forget = jnp.log1p(-in_gate)
    query_rows = queries.astype(jnp.float32).reshape(head_shape)
    value_rows = inputs.reshape(head_shape).astype(jnp.float32)

    def to_blocks(array):
        return array.reshape(SEQS, N_SP, POS_DEV, HEADS, HEAD).transpose(1, 0, 2, 3, 4)
    causal = jnp.tril(jnp.ones((POS_DEV, POS_DEV), dtype=bool))
    highest = lax.Precision.HIGHEST

    def advance(carry_state, block_inputs):
        block_query, block_gate, block_forget, block_value = block_inputs
        cumulative = jnp.cumsum(block_forget, axis=1)
        final_sum = cumulative[:, -1]
        grown = (block_query * jnp.exp(cumulative)).astype(jnp.bfloat16).astype(jnp.float32)
        shrunk = (block_gate * jnp.exp(-cumulative)).astype(jnp.bfloat16).astype(jnp.float32)
        weighted = (block_gate * jnp.exp(final_sum[:, None] - cumulative)).astype(jnp.bfloat16).astype(jnp.float32)
        scores = jnp.einsum('sthk,suhk->shtu', grown, shrunk, precision=highest)
        scores = jnp.where(causal, scores, 0.0).astype(jnp.bfloat16).astype(jnp.float32)
        carried_low = carry_state.astype(jnp.bfloat16).astype(jnp.float32)
        block_out = jnp.einsum('shtu,suhv->sthv', scores, block_value, precision=highest)
        block_out = block_out + jnp.einsum('sthk,shkv->sthv', grown, carried_low, precision=highest)
        new_state = jnp.exp(final_sum)[..., None] * carry_state + jnp.einsum('suhk,suhv->shkv', weighted, block_value, precision=highest)
        return (new_state, block_out)
    start_state = jnp.zeros((SEQS, HEADS, HEAD, HEAD), jnp.float32)
    blocks = (to_blocks(query_rows), to_blocks(in_gate), to_blocks(log_forget), to_blocks(value_rows))
    final_state, block_outs = lax.scan(advance, start_state, blocks)
    rec_raw = block_outs.transpose(1, 0, 2, 3, 4).reshape(head_shape)
    rec_norm = rec_raw * lax.rsqrt(lax.optimization_barrier(jnp.mean(rec_raw * rec_raw, axis=-1, keepdims=True)) + EPS) * head_gain.reshape(HEADS, HEAD)
    rec_out = (rec_norm.reshape(SEQS, SEQ_LEN, D_HG) * jax.nn.silu(out_gate.astype(jnp.float32))).astype(jnp.bfloat16)
    conv_part = jnp.dot(conv_out.reshape(SEQS * SEQ_LEN, D_CONV), conv_out_w, preferred_element_type=jnp.float32)
    rec_part = jnp.dot(rec_out.reshape(SEQS * SEQ_LEN, D_HG), rec_out_w, preferred_element_type=jnp.float32)
    return (conv_part + rec_part).astype(jnp.bfloat16).reshape(SEQS, SEQ_LEN, D)
```

```python
import functools

import jax
import jax.numpy as jnp
from jax import lax
from jax.experimental import pallas as pl
from jax.experimental.pallas import tpu as pltpu
from jax.sharding import PartitionSpec as P

HEAD = 128
LANES = 128
EDGE = 32
PACK = 16
COLS = 256
EPS = 1e-06
MESH = pl.DeviceIdType.MESH
F32 = jnp.float32
BF16 = jnp.bfloat16


def flip(index, mask):
    out, bit = index, 1
    while bit <= mask:
        if mask & bit:
            out = out + bit - 2 * bit * ((index // bit) % 2)
        bit *= 2
    return out


def mm(a, b, dims=((1,), (0,))):
    return lax.dot_general(a, b, (dims, ((), ())), preferred_element_type=F32)


def split3(value):
    hi = value.astype(BF16)
    rest = value - hi.astype(F32)
    mid = rest.astype(BF16)
    return hi, mid, (rest - mid.astype(F32)).astype(BF16)


def kernel(
    cfg,
    frames, norm_gain, cvw, cgw, taps, conv_bias, channel_gain, channel_shift,
    qw, fw, iw, gw, rate, head_gain, cow, row,
    out,
    gath, norm_v, wf, wi, wc, wq, wg, taps_v, cb_v, cg_v, cs_v, rate_v, hg_v, ow,
    nrm, ecum_s, gated, edges, ext, filt, stat, stat_in, cvo, rco,
    grown_s, shrunk_s, value_s, gate_s, local_s, st, st_in, carry_out, carry_in, acc, psend, precv,
    up, loc_sem, d2_send, d2_recv, fr_send, fr_recv, ed_send, ed_recv, stt_send, stt_recv,
    ca_send, ca_recv, sm_send, sm_recv, pt_send, pt_recv,
):
    n_tp, n_sp, d_conv, seq_total, owners = cfg
    positions = frames.shape[1]
    conv_n, rec_n = cvw.shape[1], qw.shape[1]
    heads = rec_n // HEAD
    nx = n_tp // 2
    chunk = carry_out.shape[2]
    stride = n_sp // owners
    pieces = acc.shape[1]
    tp, sp = lax.axis_index("tp"), lax.axis_index("sp")
    core = tp % 2
    owner = sp // stride

    barrier = pltpu.get_barrier_semaphore()
    pl.semaphore_signal(barrier, inc=1, device_id={"tp": flip(tp, 1)}, device_id_type=MESH)
    for k in range(1, nx):
        pl.semaphore_signal(barrier, inc=1, device_id={"tp": flip(tp, 2 * k)}, device_id_type=MESH)
    for d in range(1, n_sp):

        @pl.when(sp + d < n_sp)
        def _():
            pl.semaphore_signal(barrier, inc=1, device_id={"sp": sp + d}, device_id_type=MESH)

    mine = pltpu.make_async_copy(frames, gath.at[pl.ds(0, 1)], loc_sem.at[0])
    gain_in = pltpu.make_async_copy(norm_gain, norm_v, loc_sem.at[1])

    def remote(src, dst, send, recv, **device):
        return pltpu.make_async_remote_copy(
            src_ref=src, dst_ref=dst, send_sem=send, recv_sem=recv, device_id=device, device_id_type=MESH
        )

    rec_at = 2 * conv_n
    table = (
        ("f", fw, wf.at[0], wf.at[1]),
        ("rate", rate, rate_v.at[0], rate_v.at[1]),
        ("i", iw, wi.at[0], wi.at[1]),
        ("cv", cvw, wc.at[0, :, pl.ds(0, conv_n)], wc.at[1, :, pl.ds(0, conv_n)]),
        ("cg", cgw, wc.at[0, :, pl.ds(conv_n, conv_n)], wc.at[1, :, pl.ds(conv_n, conv_n)]),
        ("q", qw, wq.at[0], wq.at[1]),
        ("g", gw, wg.at[0], wg.at[1]),
        ("taps", taps, taps_v.at[0], taps_v.at[1]),
        ("cb", conv_bias, cb_v.at[0], cb_v.at[1]),
        ("gain", channel_gain, cg_v.at[0], cg_v.at[1]),
        ("shift", channel_shift, cs_v.at[0], cs_v.at[1]),
        ("hg", head_gain, hg_v.at[0], hg_v.at[1]),
        ("co", cow, ow.at[pl.ds(0, conv_n)], ow.at[pl.ds(conv_n, conv_n)]),
        ("ro", row, ow.at[pl.ds(rec_at, rec_n)], ow.at[pl.ds(rec_at + rec_n, rec_n)]),
    )
    names = [entry[0] for entry in table]
    load = {}
    swap = {}
    for n, (name, ref, here, there) in enumerate(table):
        load[name] = pltpu.make_async_copy(ref, here, loc_sem.at[2 + n])
        swap[name] = remote(here, there, d2_send.at[n], d2_recv.at[n], tp=flip(tp, 1))
    mine.start()
    gain_in.start()
    for name in names:
        load[name].start()

    fr = [None] * nx
    for k in range(1, nx):
        fr[k] = remote(gath.at[0], gath.at[k], fr_send.at[k], fr_recv.at[k], tp=flip(tp, 2 * k))

    mine.wait()
    pl.semaphore_wait(barrier, nx + sp)

    @pl.when(core == 0)
    def _():
        for k in range(1, nx):
            fr[k].start()

    for d in range(1, n_sp):

        @pl.when(sp >= d)
        def _():
            pl.semaphore_signal(up, inc=1, device_id={"sp": sp - d}, device_id_type=MESH)

    for name in names:
        load[name].wait()
        swap[name].start()
    gain_in.wait()

    t_row = lax.broadcasted_iota(jnp.int32, (positions, positions), 0)
    t_col = lax.broadcasted_iota(jnp.int32, (positions, positions), 1)
    causal = t_col <= t_row
    lower = jnp.where(causal, 1.0, 0.0).astype(BF16)
    lower3 = jnp.concatenate([lower, lower, lower], axis=1)
    tile_row = lax.broadcasted_iota(jnp.int32, (PACK, HEAD), 0)

    def norm(k):
        x = gath[k].astype(F32)
        mean = jnp.mean(x * x, axis=-1, keepdims=True)
        nrm[k] = (x * lax.rsqrt(mean + EPS) * norm_v[...]).astype(BF16)

    def project(k, weight):
        return mm(nrm[k], weight[...]).astype(BF16)

    def lanes_of(half):
        return slice(half * rec_n, (half + 1) * rec_n)

    def states(k, half):
        cols = lanes_of(half)
        forget_raw = project(k, wf.at[half]).astype(F32)
        in_gate = (rate_v[half] / seq_total) * jax.nn.sigmoid(-forget_raw)
        hi, mid, low = split3(jnp.log1p(-in_gate))
        cumulative = mm(lower3, jnp.concatenate([hi, mid, low], axis=0))
        last = cumulative[positions - 1 : positions, :]
        weighted = (in_gate * jnp.exp(last - cumulative)).astype(BF16)
        value = project(k, wi.at[half])
        value_s[k, :, cols] = value
        last_decay = jnp.exp(last)
        for h in range(heads):
            lanes = slice(h * HEAD, (h + 1) * HEAD)
            block = mm(value[:, lanes], weighted[:, lanes], ((0,), (0,))).astype(BF16)
            hi, mid, low = split3(last_decay[:, lanes])
            rows = jnp.where(
                tile_row == 0, hi.astype(F32), jnp.where(tile_row == 1, mid.astype(F32), low.astype(F32))
            ).astype(BF16)
            for r in range(HEAD // chunk):
                n = (half * heads + h) * (HEAD // chunk) + r
                st[k, n, 0:chunk] = block[r * chunk : (r + 1) * chunk]
                st[k, n, chunk : chunk + PACK] = rows
        shrunk_s[k, :, cols] = (in_gate * jnp.exp(-cumulative)).astype(BF16)
        ecum_s[k, :, cols] = jnp.exp(cumulative)

    def gates(k, half):
        both = project(k, wc.at[half]).astype(F32)
        result = (both[:, :conv_n] * jax.nn.sigmoid(both[:, conv_n:])).astype(BF16)
        cols = slice(half * conv_n, (half + 1) * conv_n)
        gated[k, :, cols] = result
        ext[k, EDGE : EDGE + positions, cols] = result.astype(F32)

    def outer(k, half):
        cols = lanes_of(half)
        queries = project(k, wq.at[half]).astype(F32)
        grown_s[k, :, cols] = (queries * ecum_s[k, :, cols]).astype(BF16)
        gate_s[k, :, cols] = project(k, wg.at[half])

    def within(k):
        for h in range(2 * heads):
            lanes = slice(h * HEAD, (h + 1) * HEAD)
            scores = mm(grown_s[k, :, lanes], shrunk_s[k, :, lanes], ((1,), (1,)))
            scores = jnp.where(causal, scores, 0.0).astype(BF16)
            local_s[k, :, lanes] = mm(scores, value_s[k, :, lanes])

    def state_copy(k, o):
        return remote(
            st.at[k, o], st_in.at[k, sp], stt_send.at[k * owners + o], stt_recv.at[k * n_sp + sp], sp=o * stride
        )

    def state_from(k, j):
        return remote(st.at[k, 0], st_in.at[k, j], stt_send.at[k * owners], stt_recv.at[k * n_sp + j], sp=j)

    def send_states(k):
        for o in range(owners):

            @pl.when(jnp.logical_and(sp != o * stride, sp < n_sp - 1))
            def _():
                state_copy(k, o).start()

    def carry_copy(k, j):
        here = pl.ds(pl.multiple_of(owner * chunk, chunk), chunk)
        return remote(
            carry_out.at[k, j], carry_in.at[k, here], ca_send.at[k * n_sp + j], ca_recv.at[k * owners + owner], sp=j
        )

    def carry_from(k, o):
        return remote(
            carry_out.at[k, 0], carry_in.at[k, pl.ds(o * chunk, chunk)],
            ca_send.at[k * n_sp], ca_recv.at[k * owners + o], sp=o * stride,
        )

    def owned(body):
        if stride == 1:
            body()
        else:
            pl.when(sp % stride == 0)(body)

    def scan(k):
        def body():
            st_in[k, sp] = st[k, owner]
            carried = jnp.zeros((chunk, HEAD), F32)
            for j in range(n_sp):
                carry_out[k, j] = carried.astype(BF16)
                if j > 0:

                    @pl.when(sp != j)
                    def _():
                        carry_copy(k, j).start()

                if j < n_sp - 1:

                    @pl.when(sp != j)
                    def _():
                        state_from(k, j).wait_recv()

                    decay = st_in[k, j, chunk : chunk + PACK].astype(F32)
                    decay = decay[0:1] + decay[1:2] + decay[2:3]
                    carried = decay * carried + st_in[k, j, 0:chunk].astype(F32)
            here = pl.multiple_of(owner * chunk, chunk)
            carry_in[k, pl.ds(here, chunk), :] = carry_out[k, sp]

        owned(body)

    def wait_carry(k):
        for o in range(owners):

            @pl.when(jnp.logical_and(sp != o * stride, sp > 0))
            def _():
                carry_from(k, o).wait_recv()

    def edge_copy(k):
        return remote(gated.at[k, pl.ds(positions - EDGE, EDGE)], edges.at[k], ed_send.at[k], ed_recv.at[k], sp=sp + 1)

    def send_edge(k):
        @pl.when(sp < n_sp - 1)
        def _():
            edge_copy(k).start()

    def stat_copy(k, j):
        return remote(
            stat.at[k], stat_in.at[j, k ^ j], sm_send.at[j * nx + k], sm_recv.at[j * nx + (k ^ j)], tp=flip(tp, 2 * j)
        )

    def stat_from(k, j):
        return remote(stat.at[k], stat_in.at[j, k], sm_send.at[j * nx + k], sm_recv.at[j * nx + k], tp=flip(tp, 2 * j))

    reach = taps.shape[0] - 1

    def conv(k):
        @pl.when(sp > 0)
        def _():
            edge_copy(k).wait_recv()
            ext[k, 0:EDGE] = edges[k].astype(F32)

        @pl.when(sp == 0)
        def _():
            ext[k, 0:EDGE] = jnp.zeros((EDGE, 2 * conv_n), F32)

        sums = squares = 0.0
        for half in range(2):
            cols = slice(half * conv_n, (half + 1) * conv_n)
            total = jnp.broadcast_to(cb_v[half], (positions, conv_n))
            tap_rows = taps_v[half].astype(F32)
            for j in range(reach + 1):
                start = EDGE - reach + j
                total = total + tap_rows[j : j + 1, :] * ext[k, start : start + positions, cols]
            filt[k, :, cols] = total
            sums = sums + jnp.sum(total, axis=-1, keepdims=True)
            squares = squares + jnp.sum(total * total, axis=-1, keepdims=True)
        lane = lax.broadcasted_iota(jnp.int32, (positions, LANES), 1)
        both = jnp.where(lane == 0, sums, jnp.where(lane == 1, squares, 0.0))
        stat[k] = jnp.transpose(both)[0:8, :]
        for j in range(1, nx):
            stat_copy(k, j).start()

    def conv_norm(k):
        both = stat[k]
        for j in range(1, nx):
            stat_from(k, j).wait_recv()
            both = both + stat_in[j, k]
        both = both / d_conv
        turned = jnp.transpose(jnp.concatenate([both, jnp.zeros((LANES - 8, positions), F32)], axis=0))
        row_mean = turned[:, 0:1]
        row_var = turned[:, 1:2] - row_mean * row_mean
        scale = lax.rsqrt(row_var + EPS)
        for half in range(2):
            cols = slice(half * conv_n, (half + 1) * conv_n)
            scaled = (filt[k, :, cols] - row_mean) * scale * cg_v[half] + cs_v[half]
            cvo[k, :, cols] = (scaled * jax.nn.sigmoid(scaled)).astype(BF16)
        for n in range(pieces):
            acc[k, n] = mm(cvo[k], ow[0:rec_at, n * COLS : (n + 1) * COLS])

    def finish(k):
        wait_carry(k)
        for h in range(2 * heads):
            lanes = slice(h * HEAD, (h + 1) * HEAD)
            rec_raw = local_s[k, :, lanes] + mm(
                grown_s[k, :, lanes], carry_in[k, h * HEAD : (h + 1) * HEAD, :], ((1,), (1,))
            )
            mean = jnp.mean(rec_raw * rec_raw, axis=-1, keepdims=True)
            gain = hg_v[h // heads][:, (h % heads) * HEAD : (h % heads + 1) * HEAD]
            rec_norm = rec_raw * lax.rsqrt(mean + EPS) * gain
            gate = gate_s[k, :, lanes].astype(F32)
            rco[k, :, lanes] = (rec_norm * (gate * jax.nn.sigmoid(gate))).astype(BF16)

    def part_copy(k, n):
        return remote(
            psend.at[k, n], precv.at[k, n], pt_send.at[k * pieces + n], pt_recv.at[k * pieces + n], tp=flip(tp, 2 * k)
        )

    def produce(k):
        for n in range(pieces):
            part = acc[k, n] + mm(rco[k], ow[rec_at : rec_at + 2 * rec_n, n * COLS : (n + 1) * COLS])
            if k == 0:
                acc[k, n] = part
            else:
                psend[k, n] = part.astype(BF16)
                part_copy(k, n).start()

    @pl.when(sp == 0)
    def _():
        carry_in[...] = jnp.zeros_like(carry_in)

    norm(0)
    states(0, 0)
    gates(0, 0)
    outer(0, 0)

    @pl.when(core == 1)
    def _():
        for k in range(1, nx):
            fr[k].start()

    for name in ("f", "rate", "i"):
        swap[name].wait_recv()
    states(0, 1)

    @pl.when(sp < n_sp - 1)
    def _():
        pl.semaphore_wait(up, n_sp - 1 - sp)

    send_states(0)
    for name in ("cv", "cg"):
        swap[name].wait_recv()
    gates(0, 1)
    send_edge(0)
    for name in ("q", "g"):
        swap[name].wait_recv()
    outer(0, 1)
    within(0)
    for name in ("taps", "cb", "gain", "shift", "hg", "co", "ro"):
        swap[name].wait_recv()

    for k in range(1, nx):
        fr[k].wait_recv()
        norm(k)
        states(k, 0)
        states(k, 1)
        send_states(k)
        gates(k, 0)
        gates(k, 1)
        send_edge(k)
        outer(k, 0)
        outer(k, 1)
        scan(k - 1)
        conv(k - 1)
        within(k)
    scan(nx - 1)
    conv(nx - 1)
    finish(0)
    for k in range(nx):
        conv_norm(k)
    for k in range(1, nx):
        finish(k)
        produce(k)
    produce(0)
    for n in range(pieces):
        total = acc[0, n]
        for k in range(1, nx):
            part_copy(k, n).wait_recv()
            total = total + precv[k, n].astype(F32)
        out[0, :, n * COLS : (n + 1) * COLS] = total.astype(BF16)

    for name in names:
        swap[name].wait_send()
    for k in range(1, nx):
        fr[k].wait_send()
        for n in range(pieces):
            part_copy(k, n).wait_send()
    for k in range(nx):
        for j in range(1, nx):
            stat_copy(k, j).wait_send()

        @pl.when(sp < n_sp - 1)
        def _():
            edge_copy(k).wait_send()

        for o in range(owners):

            @pl.when(jnp.logical_and(sp != o * stride, sp < n_sp - 1))
            def _():
                state_copy(k, o).wait_send()

        def drain():
            for j in range(1, n_sp):

                @pl.when(sp != j)
                def _():
                    carry_copy(k, j).wait_send()

        owned(drain)


def wide(array, axis):
    extra = -array.shape[axis] % LANES
    if extra == 0:
        return array
    pads = [(0, 0)] * array.ndim
    pads[axis] = (0, extra)
    return jnp.pad(array, pads)


def local(
    n_tp, n_sp, frames, norm_gain, conv_value_w, conv_gate_w, conv_taps, conv_bias, channel_gain, channel_shift,
    query_w, forget_w, input_w, gate_w, memory_rate, head_gain, conv_out_w, rec_out_w,
):
    d_conv = conv_value_w.shape[1] * n_tp
    spt, positions, depth = frames.shape
    conv_value_w, conv_gate_w, conv_taps = (wide(a, 1) for a in (conv_value_w, conv_gate_w, conv_taps))
    conv_bias, channel_gain, channel_shift, conv_out_w = (
        wide(a, 0) for a in (conv_bias, channel_gain, channel_shift, conv_out_w)
    )
    conv_n, rec_n = conv_value_w.shape[1], query_w.shape[1]
    out_n = rec_out_w.shape[1]
    assert spt == 1 and n_tp % 2 == 0 and positions == LANES and out_n % COLS == 0
    nx = n_tp // 2
    state_rows = 2 * rec_n
    owners = min(n_sp, state_rows // PACK)
    chunk = state_rows // owners
    pieces = out_n // COLS
    vm = pltpu.VMEM
    sem = pltpu.SemaphoreType.DMA
    scratch = [
        vm((nx, positions, depth), BF16),
        vm((1, depth), F32),
        vm((2, depth, rec_n), BF16),
        vm((2, depth, rec_n), BF16),
        vm((2, depth, 2 * conv_n), BF16),
        vm((2, depth, rec_n), BF16),
        vm((2, depth, rec_n), BF16),
        vm((2,) + conv_taps.shape, BF16),
        vm((2, 1, conv_n), F32),
        vm((2, 1, conv_n), F32),
        vm((2, 1, conv_n), F32),
        vm((2, 1, rec_n), F32),
        vm((2, 1, rec_n), F32),
        vm((2 * conv_n + 2 * rec_n, out_n), BF16),
        vm((nx, positions, depth), BF16),
        vm((nx, positions, 2 * rec_n), F32),
        vm((nx, positions, 2 * conv_n), BF16),
        vm((nx, EDGE, 2 * conv_n), BF16),
        vm((nx, EDGE + positions, 2 * conv_n), F32),
        vm((nx, positions, 2 * conv_n), F32),
        vm((nx, 8, positions), F32),
        vm((nx, nx, 8, positions), F32),
        vm((nx, positions, 2 * conv_n), BF16),
        vm((nx, positions, 2 * rec_n), BF16),
        vm((nx, positions, 2 * rec_n), BF16),
        vm((nx, positions, 2 * rec_n), BF16),
        vm((nx, positions, 2 * rec_n), BF16),
        vm((nx, positions, 2 * rec_n), BF16),
        vm((nx, positions, 2 * rec_n), F32),
        vm((nx, owners, chunk + PACK, HEAD), BF16),
        vm((nx, n_sp, chunk + PACK, HEAD), BF16),
        vm((nx, n_sp, chunk, HEAD), BF16),
        vm((nx, state_rows, HEAD), BF16),
        vm((nx, pieces, positions, COLS), F32),
        vm((nx, pieces, positions, COLS), BF16),
        vm((nx, pieces, positions, COLS), BF16),
        pltpu.SemaphoreType.REGULAR,
        sem((16,)),
        sem((14,)), sem((14,)),
        sem((nx,)), sem((nx,)),
        sem((nx,)), sem((nx,)),
        sem((nx * owners,)), sem((nx * n_sp,)),
        sem((nx * n_sp,)), sem((nx * owners,)),
        sem((nx * nx,)), sem((nx * nx,)),
        sem((nx * pieces,)), sem((nx * pieces,)),
    ]
    return pl.pallas_call(
        functools.partial(kernel, (n_tp, n_sp, d_conv, positions * n_sp, owners)),
        out_shape=jax.ShapeDtypeStruct((spt, positions, out_n), BF16),
        in_specs=[pl.BlockSpec(memory_space=pltpu.HBM)] * 16,
        out_specs=pl.BlockSpec(memory_space=pltpu.VMEM),
        scratch_shapes=scratch,
        compiler_params=pltpu.CompilerParams(
            collective_id=0, has_side_effects=True, vmem_limit_bytes=56 * 1024 * 1024
        ),
    )(
        frames, norm_gain[None], conv_value_w, conv_gate_w, conv_taps, conv_bias[None], channel_gain[None],
        channel_shift[None], query_w, forget_w, input_w, gate_w, memory_rate[None], head_gain[None],
        conv_out_w, rec_out_w,
    )


def solution(mesh):
    placed = (
        P("tp", "sp", None),
        P(),
        P(None, "tp"),
        P(None, "tp"),
        P(None, "tp"),
        P("tp"),
        P("tp"),
        P("tp"),
        P(None, "tp"),
        P(None, "tp"),
        P(None, "tp"),
        P(None, "tp"),
        P("tp"),
        P("tp"),
        P("tp", None),
        P("tp", None),
    )
    return jax.shard_map(
        functools.partial(local, mesh.shape["tp"], mesh.shape["sp"]),
        mesh=mesh, in_specs=placed, out_specs=P("tp", "sp", None), check_vma=False,
    )
```

```python
import functools

import jax
import jax.numpy as jnp
from jax import lax
from jax.experimental import pallas as pl
from jax.experimental.pallas import tpu as pltpu
from jax.sharding import PartitionSpec as P

HEAD = 128
LANES = 128
EDGE = 32
PACK = 16
SUB = 8
COLS = 256
EPS = 1e-06
MESH = pl.DeviceIdType.MESH
F32 = jnp.float32
BF16 = jnp.bfloat16


def flip(index, mask):
    out, bit = index, 1
    while bit <= mask:
        if mask & bit:
            out = out + bit - 2 * bit * ((index // bit) % 2)
        bit *= 2
    return out


def mm(a, b, dims=((1,), (0,))):
    return lax.dot_general(a, b, (dims, ((), ())), preferred_element_type=F32)


def split3(value):
    hi = value.astype(BF16)
    rest = value - hi.astype(F32)
    mid = rest.astype(BF16)
    return hi, mid, (rest - mid.astype(F32)).astype(BF16)


def kernel(
    cfg,
    frames, norm_gain, cvw, cgw, taps, conv_bias, channel_gain, channel_shift,
    qw, fw, iw, gw, rate, head_gain, cow, row,
    out,
    gath, norm_v, wfi, wc, wqg, taps_v, chan_v, head_v, ow,
    nrm, pacc, gate_in_s, cum_s, gated, edges, ext, filt, stat, stat_in, cvo, rco,
    grown_s, shrunk_s, value_s, gate_s, local_s, st, st_in, dec, dec_in, carry_out, carry_in, carried_s, acc, psend, precv,
    up, go, loc_sem, d2_send, d2_recv, fr_send, fr_recv, ed_send, ed_recv, stt_send, stt_recv, dc_send, dc_recv,
    ca_send, ca_recv, sm_send, sm_recv, pt_send, pt_recv,
):
    n_tp, n_sp, d_conv, seq_total, owners = cfg
    positions = frames.shape[1]
    conv_n, rec_n = cvw.shape[1], qw.shape[1]
    heads = rec_n // HEAD
    nx = n_tp // 2
    chunk = carry_out.shape[2]
    stride = n_sp // owners
    pieces = acc.shape[1]
    steps, slab = nrm.shape[1], nrm.shape[3]
    gate_at = max(steps - 2, 0)
    tp, sp = lax.axis_index("tp"), lax.axis_index("sp")
    core = tp % 2
    owner = sp // stride

    barrier = pltpu.get_barrier_semaphore()
    pl.semaphore_signal(barrier, inc=1, device_id={"tp": flip(tp, 1)}, device_id_type=MESH)
    for k in range(1, nx):
        pl.semaphore_signal(barrier, inc=1, device_id={"tp": flip(tp, 2 * k)}, device_id_type=MESH)
    for d in range(1, n_sp):

        @pl.when(sp + d < n_sp)
        def _():
            pl.semaphore_signal(barrier, inc=1, device_id={"sp": sp + d}, device_id_type=MESH)

    mine = pltpu.make_async_copy(frames, gath, loc_sem.at[0])
    gain_in = pltpu.make_async_copy(norm_gain, norm_v, loc_sem.at[1])

    def remote(src, dst, send, recv, **device):
        return pltpu.make_async_remote_copy(
            src_ref=src, dst_ref=dst, send_sem=send, recv_sem=recv, device_id=device, device_id_type=MESH
        )

    rec_at = 2 * conv_n
    own_rows = conv_n + rec_n
    table = {
        "fi": (wfi, ((fw, wfi.at[0, 0]), (iw, wfi.at[0, 1]))),
        "head": (head_v, ((rate, head_v.at[0, 0]), (head_gain, head_v.at[0, 1]))),
        "c": (wc, ((cvw, wc.at[0, :, pl.ds(0, conv_n)]), (cgw, wc.at[0, :, pl.ds(conv_n, conv_n)]))),
        "qg": (wqg, ((qw, wqg.at[0, 0]), (gw, wqg.at[0, 1]))),
        "taps": (taps_v, ((taps, taps_v.at[0]),)),
        "chan": (chan_v, ((conv_bias, chan_v.at[0, 0]), (channel_gain, chan_v.at[0, 1]), (channel_shift, chan_v.at[0, 2]))),
    }
    names = list(table)
    load, loaded, swap = [], {}, {}
    for n, (name, (buffer, parts)) in enumerate(table.items()):
        for ref, here in parts:
            load.append(pltpu.make_async_copy(ref, here, loc_sem.at[2 + n]))
        loaded[name] = pltpu.make_async_copy(buffer.at[1], buffer.at[0], loc_sem.at[2 + n])
        swap[name] = remote(buffer.at[0], buffer.at[1], d2_send.at[n], d2_recv.at[n], tp=flip(tp, 1))
    n = len(names)
    load.append(pltpu.make_async_copy(cow, ow.at[pl.ds(0, conv_n)], loc_sem.at[2 + n]))
    load.append(pltpu.make_async_copy(row, ow.at[pl.ds(rec_at, rec_n)], loc_sem.at[2 + n]))
    out_loaded = pltpu.make_async_copy(ow.at[pl.ds(0, own_rows)], ow.at[pl.ds(own_rows, own_rows)], loc_sem.at[2 + n])
    out_swap = [
        remote(ow.at[pl.ds(at, rows)], ow.at[pl.ds(at + rows, rows)], d2_send.at[n], d2_recv.at[n], tp=flip(tp, 1))
        for at, rows in ((0, conv_n), (rec_at, rec_n))
    ]
    out_swapped = remote(
        ow.at[pl.ds(0, own_rows)], ow.at[pl.ds(own_rows, own_rows)], d2_send.at[n], d2_recv.at[n], tp=flip(tp, 1)
    )
    mine.start()
    gain_in.start()
    for copy in load:
        copy.start()

    def normed_copy(k, c):
        return remote(
            nrm.at[0, c], nrm.at[k, c], fr_send.at[int(c > gate_at)], fr_recv.at[(k - 1) * steps + c], tp=flip(tp, 2 * k)
        )

    def sent(ref, sem):
        return remote(ref, ref, sem, sem, tp=flip(tp, 1))

    def normed_sent(late):
        count = steps - 1 - gate_at if late else gate_at + 1
        return sent(nrm.at[pl.ds(0, nx - 1), pl.ds(0, count)], fr_send.at[late])

    def send_normed():
        for k in range(1, nx):
            for c in range(steps):
                normed_copy(k, c).start()

    mine.wait()
    gain_in.wait()
    x = gath[0].astype(F32)
    mean = jnp.mean(x * x, axis=-1, keepdims=True)
    x = (x * lax.rsqrt(mean + EPS) * norm_v[...]).astype(BF16)
    for c in range(steps):
        nrm[0, c] = x[:, c * slab : (c + 1) * slab]
    pl.semaphore_wait(barrier, nx + sp)

    @pl.when(core == 0)
    def _():
        send_normed()

    for d in range(1, n_sp):

        @pl.when(sp >= d)
        def _():
            pl.semaphore_signal(up, inc=1, device_id={"sp": sp - d}, device_id_type=MESH)

    for name in names:
        loaded[name].wait()
        swap[name].start()
    out_loaded.wait()
    for copy in out_swap:
        copy.start()

    t_row = lax.broadcasted_iota(jnp.int32, (positions, positions), 0)
    t_col = lax.broadcasted_iota(jnp.int32, (positions, positions), 1)
    causal = t_col <= t_row
    lower = jnp.where(causal, 1.0, 0.0).astype(BF16)
    lower3 = jnp.concatenate([lower, lower, lower], axis=1)

    def weight(name, half, rows):
        if name == "c":
            return wc[half, rows, :]
        return wfi[half, "fi".index(name), rows, :] if name in "fi" else wqg[half, "qg".index(name), rows, :]

    places = {}
    for n, name in enumerate("fi"):
        for half in range(2):
            places[name, half] = slice((2 * n + half) * rec_n, (2 * n + half + 1) * rec_n)

    def slab_product(k, name, half, c):
        return mm(nrm[k, c], weight(name, half, slice(c * slab, (c + 1) * slab)))

    def feed(k, c):
        for (name, half), cols in places.items():
            part = slab_product(k, name, half, c)
            pacc[k - 1, :, cols] = part if c == 0 else pacc[k - 1, :, cols] + part

    def project(k, name, half):
        if k == 0 or (name, half) not in places:
            total = slab_product(k, name, half, 0)
            for c in range(1, steps):
                total = total + slab_product(k, name, half, c)
        else:
            total = pacc[k - 1, :, places[name, half]] + slab_product(k, name, half, steps - 1)
        return total.astype(BF16)

    def lanes_of(half):
        return slice(half * rec_n, (half + 1) * rec_n)

    def states(k, halves):
        raws = [project(k, "f", half) for half in halves]
        values = [project(k, "i", half) for half in halves]
        for half, forget_raw, value in zip(halves, raws, values):
            cols = lanes_of(half)
            in_gate = (head_v[half, 0] / seq_total) * jax.nn.sigmoid(-forget_raw.astype(F32))
            hi, mid, low = split3(jnp.log1p(-in_gate))
            cumulative = mm(lower3, jnp.concatenate([hi, mid, low], axis=0))
            last = cumulative[positions - 1 : positions, :]
            weighted = (in_gate * jnp.exp(last - cumulative)).astype(BF16)
            value_s[k, :, cols] = value
            last_decay = jnp.exp(last)
            for h in range(heads):
                lanes = slice(h * HEAD, (h + 1) * HEAD)
                block = mm(value[:, lanes], weighted[:, lanes], ((0,), (0,))).astype(BF16)
                for r in range(HEAD // chunk):
                    n = (half * heads + h) * (HEAD // chunk) + r
                    st[k, n] = block[r * chunk : (r + 1) * chunk]
                    dec[k, n] = last_decay[:, lanes]
            gate_in_s[k, :, cols] = in_gate
            cum_s[k, :, cols] = cumulative

    def gates(k, half):
        both = project(k, "c", half).astype(F32)
        result = (both[:, :conv_n] * jax.nn.sigmoid(both[:, conv_n:])).astype(BF16)
        cols = slice(half * conv_n, (half + 1) * conv_n)
        gated[k, :, cols] = result
        ext[k, half, EDGE : EDGE + positions] = result.astype(F32)

    def outer(k, half):
        cols = lanes_of(half)
        queries = project(k, "q", half).astype(F32)
        cumulative = cum_s[k, :, cols]
        grown_s[k, :, cols] = (queries * jnp.exp(cumulative)).astype(BF16)
        shrunk_s[k, :, cols] = (gate_in_s[k, :, cols] * jnp.exp(-cumulative)).astype(BF16)
        gate_s[k, :, cols] = project(k, "g", half)

    def within(k):
        for h in range(2 * heads):
            lanes = slice(h * HEAD, (h + 1) * HEAD)
            scores = mm(grown_s[k, :, lanes], shrunk_s[k, :, lanes], ((1,), (1,)))
            scores = jnp.where(causal, scores, 0.0).astype(BF16)
            local_s[k, :, lanes] = mm(scores, value_s[k, :, lanes])

    def slot(k, j):
        return 0 if k == 0 else 1 + (k - 1) * n_sp + j

    def state_copy(k, o):
        return remote(st.at[k, o], st_in.at[k, sp], stt_send.at[k], stt_recv.at[slot(k, sp)], sp=o * stride)

    def decay_copy(k, o):
        return remote(dec.at[k, o], dec_in.at[k, sp], dc_send.at[k], dc_recv.at[slot(k, sp)], sp=o * stride)

    def state_from(k, j):
        return remote(st.at[k, 0], st_in.at[k, j], stt_send.at[k], stt_recv.at[slot(k, j)], sp=j)

    def decay_from(k, j):
        return remote(dec.at[k, 0], dec_in.at[k, j], dc_send.at[k], dc_recv.at[slot(k, j)], sp=j)

    def wait_all(k):
        for last, count in ((False, n_sp - 2), (True, n_sp - 1)):

            @pl.when((sp == n_sp - 1) == last)
            def _():
                for ref, sem in ((st_in, stt_recv), (dec_in, dc_recv)):
                    some = ref.at[k, pl.ds(0, count)]
                    remote(some, some, sem.at[slot(k, 0)], sem.at[slot(k, 0)], sp=0).wait_recv()

    def send_states(k):
        for o in range(owners):

            @pl.when(jnp.logical_and(sp != o * stride, sp < n_sp - 1))
            def _():
                state_copy(k, o).start()
                decay_copy(k, o).start()

    def carry_copy(k, j):
        here = pl.ds(pl.multiple_of(owner * chunk, chunk), chunk)
        return remote(carry_out.at[k, j], carry_in.at[k, here], ca_send.at[k], ca_recv.at[k], sp=j)

    def owned(body):
        if stride == 1:
            body()
        else:
            pl.when(sp % stride == 0)(body)

    def scan(k, first, stop):
        def body():
            if first == 0:
                st_in[k, sp] = st[k, owner]
                dec_in[k, sp] = dec[k, owner]
                carried = jnp.zeros((chunk, HEAD), F32)
                if k == 0:
                    wait_all(k)
            else:
                carried = carried_s[k]
            for j in range(first, stop):
                carry_out[k, j] = carried.astype(BF16)
                if j > 0:

                    @pl.when(sp != j)
                    def _():
                        carry_copy(k, j).start()

                if j < n_sp - 1:
                    if k > 0:

                        @pl.when(sp != j)
                        def _():
                            state_from(k, j).wait_recv()
                            decay_from(k, j).wait_recv()

                    carried = dec_in[k, j] * carried + st_in[k, j].astype(F32)
            if stop < n_sp:
                carried_s[k] = carried
            else:
                here = pl.multiple_of(owner * chunk, chunk)
                carry_in[k, pl.ds(here, chunk), :] = carry_out[k, sp]

        owned(body)

    def wait_carry(k):
        for count, mine in ((owners - 1, True), (owners, False)):

            @pl.when(jnp.logical_and(sp > 0, (sp % stride == 0) == mine))
            def _():
                some = carry_in.at[k, pl.ds(0, count * chunk)]
                remote(some, some, ca_recv.at[k], ca_recv.at[k], sp=0).wait_recv()

    def edge_copy(k):
        return remote(gated.at[k, pl.ds(positions - EDGE, EDGE)], edges.at[k], ed_send.at[k], ed_recv.at[k], sp=sp + 1)

    def send_edge(k):
        @pl.when(sp < n_sp - 1)
        def _():
            edge_copy(k).start()

    def stat_copy(k, j):
        return remote(
            stat.at[k], stat_in.at[j, k ^ j], sm_send.at[0], sm_recv.at[(j - 1) * nx + (k ^ j)], tp=flip(tp, 2 * j)
        )

    def stat_from(k, j):
        return remote(stat.at[k], stat_in.at[j, k], sm_send.at[0], sm_recv.at[(j - 1) * nx + k], tp=flip(tp, 2 * j))

    reach = taps.shape[0] - 1

    def conv(k):
        @pl.when(sp > 0)
        def _():
            edge_copy(k).wait_recv()
            for half in range(2):
                cols = slice(half * conv_n, (half + 1) * conv_n)
                ext[k, half, 0:EDGE] = edges[k, :, cols].astype(F32)

        @pl.when(sp == 0)
        def _():
            ext[k, :, 0:EDGE] = jnp.zeros((2, EDGE, conv_n), F32)

        sums = squares = 0.0
        for half in range(2):
            cols = slice(half * conv_n, (half + 1) * conv_n)
            total = jnp.broadcast_to(chan_v[half, 0], (positions, conv_n))
            tap_rows = taps_v[half].astype(F32)
            for shift in range(SUB):
                part = None
                for start in range(EDGE - reach, EDGE + 1):
                    if start % SUB == shift:
                        low, rows = start - shift, positions + (SUB if shift else 0)
                        j = start - EDGE + reach
                        term = tap_rows[j : j + 1, :] * ext[k, half, low : low + rows]
                        part = term if part is None else part + term
                if part is not None:
                    total = total + part[shift : shift + positions]
            filt[k, :, cols] = total
            sums = sums + jnp.sum(total, axis=-1, keepdims=True)
            squares = squares + jnp.sum(total * total, axis=-1, keepdims=True)
        lane = lax.broadcasted_iota(jnp.int32, (positions, LANES), 1)
        both = jnp.where(lane == 0, sums, jnp.where(lane == 1, squares, 0.0))
        stat[k] = jnp.transpose(both)[0:8, :]
        for j in range(1, nx):
            stat_copy(k, j).start()

    def conv_norm(k):
        both = stat[k]
        for j in range(1, nx):
            stat_from(k, j).wait_recv()
            both = both + stat_in[j, k]
        both = both / d_conv
        turned = jnp.transpose(jnp.concatenate([both, jnp.zeros((LANES - 8, positions), F32)], axis=0))
        row_mean = turned[:, 0:1]
        row_var = turned[:, 1:2] - row_mean * row_mean
        scale = lax.rsqrt(row_var + EPS)
        for half in range(2):
            cols = slice(half * conv_n, (half + 1) * conv_n)
            scaled = (filt[k, :, cols] - row_mean) * scale * chan_v[half, 1] + chan_v[half, 2]
            cvo[k, :, cols] = (scaled * jax.nn.sigmoid(scaled)).astype(BF16)
        for n in range(pieces):
            acc[k, n] = mm(cvo[k], ow[0:rec_at, n * COLS : (n + 1) * COLS])

    def finish(k):
        wait_carry(k)
        for h in range(2 * heads):
            lanes = slice(h * HEAD, (h + 1) * HEAD)
            rec_raw = local_s[k, :, lanes] + mm(
                grown_s[k, :, lanes], carry_in[k, h * HEAD : (h + 1) * HEAD, :], ((1,), (1,))
            )
            mean = jnp.mean(rec_raw * rec_raw, axis=-1, keepdims=True)
            gain = head_v[h // heads, 1][:, (h % heads) * HEAD : (h % heads + 1) * HEAD]
            rec_norm = rec_raw * lax.rsqrt(mean + EPS) * gain
            gate = gate_s[k, :, lanes].astype(F32)
            rco[k, :, lanes] = (rec_norm * (gate * jax.nn.sigmoid(gate))).astype(BF16)

    def part_copy(k, n):
        return remote(
            psend.at[k, n], precv.at[k, n], pt_send.at[0], pt_recv.at[(k - 1) * pieces + n], tp=flip(tp, 2 * k)
        )

    def produce(k):
        for n in range(pieces):
            part = acc[k, n] + mm(rco[k], ow[rec_at : rec_at + 2 * rec_n, n * COLS : (n + 1) * COLS])
            if k == 0:
                acc[k, n] = part
            else:
                psend[k, n] = part.astype(BF16)
                part_copy(k, n).start()

    @pl.when(sp == 0)
    def _():
        carry_in[...] = jnp.zeros_like(carry_in)

    states(0, (0,))
    gates(0, 0)
    outer(0, 0)
    if nx > 1:

        @pl.when(core == 0)
        def _():
            normed_sent(0).wait_send()
            pl.semaphore_signal(go, inc=1, device_id={"tp": flip(tp, 1)}, device_id_type=MESH)

        @pl.when(core == 1)
        def _():
            pl.semaphore_wait(go, 1)
            send_normed()

    for name in ("fi", "head"):
        swap[name].wait_recv()
    states(0, (1,))

    @pl.when(sp < n_sp - 1)
    def _():
        pl.semaphore_wait(up, n_sp - 1 - sp)

    swap["c"].wait_recv()
    gates(0, 1)
    send_edge(0)
    send_states(0)

    def rest():
        swap["qg"].wait_recv()
        outer(0, 1)
        within(0)
        for copy in (swap["taps"], swap["chan"], out_swapped):
            copy.wait_recv()

    pl.when(core == 1)(rest)
    for k in range(1, nx):
        for c in range(steps - 1):
            normed_copy(k, c).wait_recv()
            feed(k, c)
        if k == 1:
            pl.when(core == 0)(rest)
        normed_copy(k, steps - 1).wait_recv()
        states(k, (0, 1))
        send_states(k)
        gates(k, 0)
        gates(k, 1)
        send_edge(k)
        middle = n_sp // 2
        late = sp >= middle
        pl.when(jnp.logical_not(late))(functools.partial(conv, k - 1))
        scan(k, 0, middle)
        pl.when(late)(functools.partial(conv, k - 1))
        scan(k, middle, n_sp)
        outer(k, 0)
        outer(k, 1)
        within(k)
    if nx == 1:
        pl.when(core == 0)(rest)
    conv(nx - 1)
    for k in range(1, nx):
        conv_norm(k)
    for k in range(1, nx):
        finish(k)
        produce(k)
    scan(0, 0, n_sp)
    conv_norm(0)
    finish(0)
    produce(0)

    for name in names:
        swap[name].wait_send()
    out_swapped.wait_send()
    for k in range(nx):

        @pl.when(sp < n_sp - 1)
        def _():
            edge_copy(k).wait_send()

        for count, mine in ((owners - 1, True), (owners, False)):

            @pl.when(jnp.logical_and(sp < n_sp - 1, (sp % stride == 0) == mine))
            def _():
                sent(st.at[k, pl.ds(0, count)], stt_send.at[k]).wait_send()
                sent(dec.at[k, pl.ds(0, count)], dc_send.at[k]).wait_send()

        for first, count in ((False, n_sp - 2), (True, n_sp - 1)):

            @pl.when(jnp.logical_and(sp % stride == 0, (sp == 0) == first))
            def _():
                sent(carry_out.at[k, pl.ds(0, count)], ca_send.at[k]).wait_send()

    if nx > 1:
        sent(stat_in.at[pl.ds(0, nx - 1)], sm_send.at[0]).wait_send()

        @pl.when(core == 1)
        def _():
            normed_sent(0).wait_send()

        normed_sent(1).wait_send()
        sent(psend.at[pl.ds(0, nx - 1)], pt_send.at[0]).wait_send()
    for n in range(pieces):
        total = acc[0, n]
        for k in range(1, nx):
            part_copy(k, n).wait_recv()
            total = total + precv[k, n].astype(F32)
        out[0, :, n * COLS : (n + 1) * COLS] = total.astype(BF16)


def wide(array, axis):
    extra = -array.shape[axis] % LANES
    if extra == 0:
        return array
    pads = [(0, 0)] * array.ndim
    pads[axis] = (0, extra)
    return jnp.pad(array, pads)


def local(
    n_tp, n_sp, frames, norm_gain, conv_value_w, conv_gate_w, conv_taps, conv_bias, channel_gain, channel_shift,
    query_w, forget_w, input_w, gate_w, memory_rate, head_gain, conv_out_w, rec_out_w,
):
    d_conv = conv_value_w.shape[1] * n_tp
    spt, positions, depth = frames.shape
    conv_value_w, conv_gate_w, conv_taps = (wide(a, 1) for a in (conv_value_w, conv_gate_w, conv_taps))
    conv_bias, channel_gain, channel_shift, conv_out_w = (
        wide(a, 0) for a in (conv_bias, channel_gain, channel_shift, conv_out_w)
    )
    conv_n, rec_n = conv_value_w.shape[1], query_w.shape[1]
    out_n = rec_out_w.shape[1]
    assert spt == 1 and n_tp % 2 == 0 and positions == LANES and out_n % COLS == 0 and depth % COLS == 0
    nx = n_tp // 2
    state_rows = 2 * rec_n
    owners = min(n_sp, state_rows // PACK)
    chunk = state_rows // owners
    pieces = out_n // COLS
    steps = depth // COLS
    vm = pltpu.VMEM
    sem = pltpu.SemaphoreType.DMA
    scratch = [
        vm((1, positions, depth), BF16),
        vm((1, depth), F32),
        vm((2, 2, depth, rec_n), BF16),
        vm((2, depth, 2 * conv_n), BF16),
        vm((2, 2, depth, rec_n), BF16),
        vm((2,) + conv_taps.shape, BF16),
        vm((2, 3, 1, conv_n), F32),
        vm((2, 2, 1, rec_n), F32),
        vm((2 * conv_n + 2 * rec_n, out_n), BF16),
        vm((nx, steps, positions, COLS), BF16),
        vm((max(nx - 1, 1), positions, 4 * rec_n), F32),
        vm((nx, positions, 2 * rec_n), F32),
        vm((nx, positions, 2 * rec_n), F32),
        vm((nx, positions, 2 * conv_n), BF16),
        vm((nx, EDGE, 2 * conv_n), BF16),
        vm((nx, 2, EDGE + positions, conv_n), F32),
        vm((nx, positions, 2 * conv_n), F32),
        vm((nx, 8, positions), F32),
        vm((nx, nx, 8, positions), F32),
        vm((nx, positions, 2 * conv_n), BF16),
        vm((nx, positions, 2 * rec_n), BF16),
        vm((nx, positions, 2 * rec_n), BF16),
        vm((nx, positions, 2 * rec_n), BF16),
        vm((nx, positions, 2 * rec_n), BF16),
        vm((nx, positions, 2 * rec_n), BF16),
        vm((nx, positions, 2 * rec_n), F32),
        vm((nx, owners, chunk, HEAD), BF16),
        vm((nx, n_sp, chunk, HEAD), BF16),
        vm((nx, owners, 1, HEAD), F32),
        vm((nx, n_sp, 1, HEAD), F32),
        vm((nx, n_sp, chunk, HEAD), BF16),
        vm((nx, state_rows, HEAD), BF16),
        vm((nx, chunk, HEAD), F32),
        vm((nx, pieces, positions, COLS), F32),
        vm((nx, pieces, positions, COLS), BF16),
        vm((nx, pieces, positions, COLS), BF16),
        pltpu.SemaphoreType.REGULAR,
        pltpu.SemaphoreType.REGULAR,
        sem((9,)),
        sem((7,)), sem((7,)),
        sem((2,)), sem((max(nx - 1, 1) * steps,)),
        sem((nx,)), sem((nx,)),
        sem((nx,)), sem((1 + (nx - 1) * n_sp,)),
        sem((nx,)), sem((1 + (nx - 1) * n_sp,)),
        sem((nx,)), sem((nx,)),
        sem((1,)), sem((max(nx - 1, 1) * nx,)),
        sem((1,)), sem((max(nx - 1, 1) * pieces,)),
    ]
    return pl.pallas_call(
        functools.partial(kernel, (n_tp, n_sp, d_conv, positions * n_sp, owners)),
        out_shape=pltpu.VMEM((spt, positions, out_n), BF16),
        in_specs=[pl.BlockSpec(memory_space=pltpu.HBM)] * 16,
        out_specs=pl.BlockSpec(memory_space=pltpu.VMEM),
        scratch_shapes=scratch,
        compiler_params=pltpu.CompilerParams(
            collective_id=0, has_side_effects=True, vmem_limit_bytes=56 * 1024 * 1024
        ),
    )(
        frames, norm_gain[None], conv_value_w, conv_gate_w, conv_taps, conv_bias[None], channel_gain[None],
        channel_shift[None], query_w, forget_w, input_w, gate_w, memory_rate[None], head_gain[None],
        conv_out_w, rec_out_w,
    )


def solution(mesh):
    placed = (
        P("tp", "sp", None),
        P(),
        P(None, "tp"),
        P(None, "tp"),
        P(None, "tp"),
        P("tp"),
        P("tp"),
        P("tp"),
        P(None, "tp"),
        P(None, "tp"),
        P(None, "tp"),
        P(None, "tp"),
        P("tp"),
        P("tp"),
        P("tp", None),
        P("tp", None),
    )
    return jax.shard_map(
        functools.partial(local, mesh.shape["tp"], mesh.shape["sp"]),
        mesh=mesh, in_specs=placed, out_specs=P("tp", "sp", None), check_vma=False,
    )
```
